32 devices in a mesh: sp: 16 (over z, y, x), tp: 2 (over core).
Axes of the slice: x: 2, y: 2, z: 4, core: 2. Of those that a mesh axis runs over, the one named last changes fastest.
Arguments:
- queries: bfloat16 [2048, 1024], P('sp', 'tp'), may hold values from -5 to 5
- keys: bfloat16 [2048, 1024], P('sp', 'tp'), may hold values from -5 to 5
- values: bfloat16 [2048, 1024], P('sp', 'tp'), may hold values from -5 to 5
- in_gate: float32 [8, 2048], P('tp', 'sp'), may hold values from -7 to 213
- forget_gate: float32 [8, 2048], P('tp', 'sp'), may hold values from 0 to 17
- stream: bfloat16 [2048, 2048], P('sp', 'tp'), may hold values from -24 to 24
- head_gain: float32 [1024], replicated, may hold values from 0.1 to 1.9
- out_weight: bfloat16 [1024, 2048], P(None, 'tp'), may hold values from -0.1875 to 0.1875
- norm_gain: float32 [2048], replicated, may hold values from 0.1 to 1.9
- gate_weight: bfloat16 [2048, 5632], P('sp', 'tp'), may hold values from -0.125 to 0.125
- up_weight: bfloat16 [2048, 5632], P('sp', 'tp'), may hold values from -0.125 to 0.125
- down_weight: bfloat16 [2048, 5632], P('sp', 'tp'), may hold values from -0.15625 to 0.15625
Outputs:
- layer_out: float32 [2048, 2048], P('sp', 'tp')
The draws below stay inside these ranges and needn't reach their ends.
All inputs are finite; a program needn't handle non-finite values.
Results may differ from the reference program's by a relative error of at most 0.004.
Values may be sent and summed in bfloat16 or wider, within the bound.
A program may use at most 128 MiB of HBM per device.

```python
import math
import jax
import jax.numpy as jnp
from jax import lax

D = 2048
FF = 5632
MEMORY_HEADS = 8
HEAD_DIM = 128
BLOCK = 128
TOK_DEV = 128
SEQUENCE_TOKENS = 2048
MIX = 1024
N_TP = 2


def draw_stream(key, part):
    noise_key, row_key = jax.random.split(key, 2)
    column = jnp.arange(D, dtype=jnp.float32) / D
    column_scale = jnp.exp(math.log(0.3) + math.log(10.0) * column)[None, :]
    base_draw = jnp.clip(jax.random.normal(noise_key, (SEQUENCE_TOKENS, D), jnp.float32), -4.0, 4.0)
    row_scale = jnp.exp(jax.random.uniform(row_key, (SEQUENCE_TOKENS, 1), jnp.float32, math.log(0.5), math.log(2.0)))
    return (base_draw * row_scale * column_scale).astype(jnp.bfloat16)


def draw_in_gate(key, part):
    noise_key = jax.random.fold_in(key, 0)
    return jnp.clip(-1.0 + 1.5 * jax.random.normal(noise_key, (MEMORY_HEADS, SEQUENCE_TOKENS), jnp.float32), -7.0, 5.0)


def draw_forget_gate(key, part):
    permute_random_key, perturb_random_key, decay_random_key, surge_random_key, retain_random_key = jax.random.split(key, 5)
    slow_level = math.log(4.0 * SEQUENCE_TOKENS)
    head_order = jax.random.permutation(permute_random_key, MEMORY_HEADS)
    fast_heads = head_order < MEMORY_HEADS // 2
    jitter = jnp.clip(jax.random.normal(perturb_random_key, (MEMORY_HEADS, SEQUENCE_TOKENS), jnp.float32), -3.0, 3.0)
    head_level = jnp.where(fast_heads, 4.5, slow_level)[:, None]
    block_rate = jax.random.uniform(decay_random_key, (MEMORY_HEADS, SEQUENCE_TOKENS // TOK_DEV), jnp.float32, 0.0, math.log(4.0))
    block_rate = jnp.repeat(block_rate, TOK_DEV, axis=1)
    gate_outputs = head_level - block_rate + jitter
    surge_position = jax.random.randint(surge_random_key, (MEMORY_HEADS, 2), 0, SEQUENCE_TOKENS)
    surge_retain = jax.random.uniform(retain_random_key, (MEMORY_HEADS, 2), jnp.float32, 0.5, 0.8)
    surge_amount = jnp.log(surge_retain / (1.0 - surge_retain))
    token_position = jnp.arange(SEQUENCE_TOKENS, dtype=jnp.int32)[None, :, None]
    surge_applied = token_position == surge_position[:, None, :]
    surge_magnitude = jnp.min(jnp.where(surge_applied, surge_amount[:, None, :], 100.0), axis=2)
    return jnp.where(jnp.any(surge_applied, axis=2), surge_magnitude, gate_outputs)


def level_of(own_key, dims, cuts, low, high):
    loudness = 1.0
    for axis_at, blocks in cuts:
        heights = jax.random.uniform(jax.random.fold_in(jax.random.fold_in(own_key, 6), axis_at), (blocks,), jnp.float32, low / len(cuts), high / len(cuts))
        loudness = loudness * jnp.repeat(jnp.exp(heights), dims[axis_at] // blocks).reshape((-1,) + (1,) * (len(dims) - 1 - axis_at))
    return loudness


def gaussian(own_key, extent, deviation, limit, shards=(), kind=jnp.bfloat16):
    level = level_of(own_key, extent, shards, -0.22, 0.18) if shards else 1.0
    values = jax.random.normal(own_key, extent, jnp.float32) * deviation * level
    return jnp.minimum(jnp.maximum(values, -limit), limit).astype(kind)


def setup_inputs(seed: int = 0) -> dict:
    key_list = jax.random.split(jax.random.key(seed), 13)
    return {
        "queries": gaussian(key_list[0], (SEQUENCE_TOKENS, MIX), 1.0, 5.0, ((0, 16), (1, 2))),
        "keys": gaussian(key_list[1], (SEQUENCE_TOKENS, MIX), 1.0, 5.0, ((0, 16), (1, 2))),
        "values": gaussian(key_list[2], (SEQUENCE_TOKENS, MIX), 1.0, 5.0, ((0, 16), (1, 2))),
        "in_gate": draw_in_gate(jax.random.fold_in(key_list[12], 71), 0),
        "forget_gate": draw_forget_gate(jax.random.fold_in(key_list[12], 71), 0),
        "stream": draw_stream(jax.random.fold_in(key_list[12], 71), 0),
        "head_gain": jnp.clip(1.0 + 0.18 * jax.random.normal(key_list[6], (MIX,), jnp.float32), 0.1, 1.9),
        "out_weight": gaussian(key_list[7], (MIX, D), MIX ** -0.5, 0.1875, ((1, 2),)),
        "norm_gain": jnp.clip(1.0 + 0.18 * jax.random.normal(key_list[8], (D,), jnp.float32), 0.1, 1.9),
        "gate_weight": gaussian(key_list[9], (D, FF), D ** -0.5, 0.125, ((0, 16), (1, 2))),
        "up_weight": gaussian(key_list[10], (D, FF), D ** -0.5, 0.125, ((0, 16), (1, 2))),
        "down_weight": gaussian(key_list[11], (D, FF), (FF // 4) ** -0.5, 0.15625, ((0, 16), (1, 2))),
    }


norm_eps = 1e-06

def reference(queries, keys, values, in_gate, forget_gate, stream, head_gain, out_weight, norm_gain, gate_weight, up_weight, down_weight):
    blocks = SEQUENCE_TOKENS // BLOCK
    key_scale = HEAD_DIM ** (-0.5)
    cumulative = jnp.cumsum(jax.nn.log_sigmoid(forget_gate).reshape(MEMORY_HEADS, blocks, BLOCK), axis=-1)
    gate_blocks = in_gate.reshape(MEMORY_HEADS, blocks, BLOCK)
    causal = lax.broadcasted_iota(jnp.int32, (BLOCK, BLOCK), 0) >= lax.broadcasted_iota(jnp.int32, (BLOCK, BLOCK), 1)

    def advance(running, section):
        memory, top_now = running
        query_blk, key_blk, value_blk, cum_blk, gate_blk = section
        block_fall = cum_blk[:, -1]
        log_weight = block_fall[:, None] - cum_blk + gate_blk
        block_top = lax.optimization_barrier(jnp.max(log_weight, axis=1))
        key_weight = jnp.exp(log_weight - block_top[:, None]) * key_scale
        weighted = (key_weight.T[:, :, None] * key_blk.astype(jnp.float32)).astype(jnp.bfloat16)
        block_memory = jnp.einsum('shd,she->hde', weighted.astype(jnp.float32), value_blk.astype(jnp.float32))
        spread = cum_blk[:, :, None] - cum_blk[:, None, :] + gate_blk[:, None, :]
        spread = jnp.where(causal, spread, -jnp.inf)
        carried = cum_blk + top_now[:, None]
        row_top = jnp.maximum(carried, lax.optimization_barrier(jnp.max(spread, axis=2)))
        decay_weight = jnp.exp(spread - row_top[:, :, None])
        scores = jnp.einsum('thd,shd->hts', query_blk.astype(jnp.float32), key_blk.astype(jnp.float32))
        weights = (scores * key_scale * decay_weight).astype(jnp.bfloat16)
        inner_part = jnp.einsum('hts,she->the', weights.astype(jnp.float32), value_blk.astype(jnp.float32))
        outer_part = jnp.einsum('thd,hde->the', query_blk.astype(jnp.float32), memory, precision=lax.Precision.HIGHEST)
        readout = jnp.exp(carried - row_top).T[:, :, None] * outer_part + inner_part
        new_top = jnp.maximum(block_fall + top_now, block_top)
        new_memory = jnp.exp(block_fall + top_now - new_top)[:, None, None] * memory + jnp.exp(block_top - new_top)[:, None, None] * block_memory
        return ((new_memory, new_top), readout)

    def split_blocks(array):
        return array.reshape(blocks, BLOCK, MEMORY_HEADS, HEAD_DIM)
    start_state = (jnp.zeros((MEMORY_HEADS, HEAD_DIM, HEAD_DIM), jnp.float32), jnp.zeros((MEMORY_HEADS,), jnp.float32))
    sections = (split_blocks(queries), split_blocks(keys), split_blocks(values), jnp.transpose(cumulative, (1, 0, 2)), jnp.transpose(gate_blocks, (1, 0, 2)))
    final_state, readouts = lax.scan(advance, start_state, sections)
    readouts = readouts.reshape(SEQUENCE_TOKENS, MEMORY_HEADS, HEAD_DIM)
    row_scale = lax.rsqrt(lax.optimization_barrier(jnp.mean(readouts * readouts, axis=-1, keepdims=True)) + norm_eps)
    heads_normed = (readouts * row_scale * head_gain.reshape(MEMORY_HEADS, HEAD_DIM)).astype(jnp.bfloat16).reshape(SEQUENCE_TOKENS, MIX)
    mixed_float = stream.astype(jnp.float32) + jnp.dot(heads_normed, out_weight, preferred_element_type=jnp.float32)
    factor = lax.rsqrt(lax.optimization_barrier(jnp.mean(mixed_float * mixed_float, axis=1, keepdims=True)) + norm_eps)
    normed = (mixed_float * factor * norm_gain).astype(jnp.bfloat16)
    group_width = FF // N_TP

    def channel_rows(row_block):
        gate_acts = jnp.dot(row_block, gate_weight, preferred_element_type=jnp.float32)
        up_acts = jnp.dot(row_block, up_weight, preferred_element_type=jnp.float32)
        hidden = (jax.nn.silu(gate_acts) * up_acts).astype(jnp.bfloat16)
        running_sum = jnp.zeros((row_block.shape[0], D), jnp.float32)
        for group_index in range(N_TP):
            lower = group_index * group_width
            partial_sum = jnp.dot(hidden[:, lower:lower + group_width], down_weight[:, lower:lower + group_width].T, preferred_element_type=jnp.float32)
            rounded = lax.optimization_barrier(partial_sum.astype(jnp.bfloat16))
            running_sum = running_sum + rounded.astype(jnp.float32)
        return running_sum
    channel = lax.map(channel_rows, normed.reshape(SEQUENCE_TOKENS // TOK_DEV, TOK_DEV, D)).reshape(SEQUENCE_TOKENS, D)
    return mixed_float + 0.5 * channel
```

```python
import jax
import jax.numpy as jnp
from jax import lax
from jax.sharding import PartitionSpec as P

D = 2048
HEAD_DIM = 128
BLOCK = 128


norm_eps = 1e-06
far_below = -1e30


def entering_state(total):
    memory, top, fall = total
    devices, here = (lax.axis_size("sp"), lax.axis_index("sp"))
    heads, rows, columns = memory.shape
    own_tops = jnp.broadcast_to(jnp.stack([top, fall])[None], (devices, 2, heads))
    tops = lax.all_to_all(own_tops, "sp", 0, 0)
    all_top, all_fall = tops[:, 0], tops[:, 1]
    index = jnp.arange(devices)
    between = (index[None, None, :] > jnp.arange(-1, devices)[None, :, None]) & (
        index[None, None, :] < index[:, None, None]
    )
    after = jnp.sum(jnp.where(between[..., None], all_fall[None, None], 0.0), axis=2)
    reach = jnp.concatenate([jnp.zeros((1, heads), jnp.float32), all_top])[None] + after
    earlier = jnp.arange(-1, devices)[None, :, None] < index[:, None, None]
    reach = jnp.where(earlier, reach, -jnp.inf)
    top_in = jnp.max(reach, axis=1)
    share = jnp.exp(reach - top_in[:, None])[:, 1:]
    pieces = lax.all_to_all(
        jnp.transpose(memory.reshape(heads, devices, rows // devices, columns), (1, 0, 2, 3)),
        "sp", 0, 0,
    )
    sums = jnp.einsum("kjh,jhde->khde", share, pieces, precision=lax.Precision.HIGHEST)
    back = lax.all_to_all(sums, "sp", 0, 0)
    memory_in = jnp.transpose(back, (1, 0, 2, 3)).reshape(heads, rows, columns)
    return (memory_in, lax.dynamic_index_in_dim(top_in, here, 0, False), jnp.zeros_like(fall))


def merge_states(earlier, later):
    memory_early, top_early, fall_early = earlier
    memory_late, top_late, fall_late = later
    new_top = jnp.maximum(fall_late + top_early, top_late)
    keep_early = jnp.exp(fall_late + top_early - new_top)
    keep_late = jnp.exp(top_late - new_top)
    memory = keep_early[..., None, None] * memory_early + keep_late[..., None, None] * memory_late
    return (memory, new_top, fall_early + fall_late)


def memory_cell(queries, keys, values, in_gate, forget_gate, own_gain):
    tokens = queries.shape[0]
    local_heads = in_gate.shape[0]
    blocks = tokens // BLOCK
    key_scale = HEAD_DIM ** (-0.5)
    query_blocks = queries.reshape(blocks, BLOCK, local_heads, HEAD_DIM)
    key_blocks = keys.reshape(blocks, BLOCK, local_heads, HEAD_DIM)
    value_blocks = values.reshape(blocks, BLOCK, local_heads, HEAD_DIM)
    gate_blocks = in_gate.reshape(local_heads, blocks, BLOCK)
    cumulative = jnp.cumsum(
        jax.nn.log_sigmoid(forget_gate).reshape(local_heads, blocks, BLOCK), axis=-1
    )
    block_fall = cumulative[..., -1]
    log_weight = block_fall[..., None] - cumulative + gate_blocks
    block_top = jnp.max(log_weight, axis=-1)
    key_weight = jnp.exp(log_weight - block_top[..., None]) * key_scale
    weighted = (jnp.transpose(key_weight, (1, 2, 0))[..., None] * key_blocks).astype(jnp.bfloat16)
    block_memory = jnp.einsum(
        "nshd,nshe->nhde", weighted, value_blocks, preferred_element_type=jnp.float32
    )
    neutral = (
        jnp.zeros((local_heads, HEAD_DIM, HEAD_DIM), jnp.float32),
        jnp.full((local_heads,), far_below, jnp.float32),
        jnp.zeros((local_heads,), jnp.float32),
    )

    def advance(running, summary):
        return (merge_states(running, summary), running)

    device_total, before_block = lax.scan(
        advance, neutral, (block_memory, block_top.T, block_fall.T)
    )
    entering = entering_state(device_total)
    memory_in, top_in, fall_in = merge_states(
        jax.tree.map(lambda member: member[None], entering), before_block
    )
    causal = lax.broadcasted_iota(jnp.int32, (BLOCK, BLOCK), 0) >= lax.broadcasted_iota(
        jnp.int32, (BLOCK, BLOCK), 1
    )
    spread = cumulative[..., :, None] - cumulative[..., None, :] + gate_blocks[..., None, :]
    spread = jnp.where(causal, spread, -jnp.inf)
    carried = cumulative + top_in.T[..., None]
    row_top = jnp.maximum(carried, jnp.max(spread, axis=-1))
    decay_weight = jnp.exp(spread - row_top[..., None])
    scores = jnp.einsum(
        "nthd,nshd->hnts", query_blocks, key_blocks, preferred_element_type=jnp.float32
    )
    weights = (scores * key_scale * decay_weight).astype(jnp.bfloat16)
    inner_part = jnp.einsum(
        "hnts,nshe->nthe", weights, value_blocks, preferred_element_type=jnp.float32
    )
    outer_part = jnp.einsum(
        "nthd,nhde->nthe",
        query_blocks.astype(jnp.float32),
        memory_in,
        precision=lax.Precision.HIGHEST,
    )
    readout = (
        jnp.transpose(jnp.exp(carried - row_top), (1, 2, 0))[..., None] * outer_part + inner_part
    )
    row_scale = lax.rsqrt(jnp.mean(readout * readout, axis=-1, keepdims=True) + norm_eps)
    head_scale = own_gain.reshape(local_heads, HEAD_DIM)
    normed_heads = (readout * row_scale * head_scale).astype(jnp.bfloat16)
    return normed_heads.reshape(tokens, local_heads * HEAD_DIM)


def local(
    queries,
    keys,
    values,
    in_gate,
    forget_gate,
    stream,
    head_gain,
    out_weight,
    norm_gain,
    gate_weight,
    up_weight,
    down_weight,
):
    column_index = lax.axis_index("tp")
    local_width = queries.shape[1]
    own_gain = lax.dynamic_slice_in_dim(head_gain, column_index * local_width, local_width)
    heads_out = memory_cell(queries, keys, values, in_gate, forget_gate, own_gain)
    columns = out_weight.shape[1]
    projected = jnp.dot(
        lax.all_gather(heads_out, "tp", axis=1, tiled=True),
        out_weight,
        preferred_element_type=jnp.float32,
    )
    mixed_stream = stream.astype(jnp.float32) + projected
    squares = lax.psum(jnp.sum(mixed_stream * mixed_stream, axis=1), "tp")
    factor = lax.rsqrt(squares / D + norm_eps)
    own_norm = lax.dynamic_slice_in_dim(norm_gain, column_index * columns, columns)
    own_normed = (mixed_stream * factor[:, None] * own_norm).astype(jnp.bfloat16)
    if 2 * own_normed.size * lax.axis_size("tp") < 3 * gate_weight.size:
        channel = move_tokens(own_normed, gate_weight, up_weight, down_weight)
    else:
        channel = move_weights(own_normed, gate_weight, up_weight, down_weight)
    return mixed_stream + 0.5 * channel


def move_tokens(own_normed, gate_weight, up_weight, down_weight):
    devices = lax.axis_size("sp")
    rows, units = gate_weight.shape
    own_units = units // devices
    weights = jnp.stack([gate_weight.T, up_weight.T, down_weight.T])
    weights = weights.reshape(3, devices, own_units, rows)
    weights = lax.all_to_all(weights, "sp", 1, 2)
    weights = weights.reshape(3, own_units, devices * rows)
    half = lax.all_gather(own_normed, "sp", axis=0, tiled=True)
    normed = lax.all_gather(half, "tp", axis=1, tiled=True)
    gate_acts = jnp.einsum("td,fd->tf", normed, weights[0], preferred_element_type=jnp.float32)
    up_acts = jnp.einsum("td,fd->tf", normed, weights[1], preferred_element_type=jnp.float32)
    hidden = (jax.nn.silu(gate_acts) * up_acts).astype(jnp.bfloat16)
    terms = jnp.einsum("tf,fd->td", hidden, weights[2], preferred_element_type=jnp.float32)
    terms = lax.psum_scatter(
        terms.astype(jnp.bfloat16), "tp", scatter_dimension=1, tiled=True
    )
    return lax.psum_scatter(terms, "sp", scatter_dimension=0, tiled=True).astype(jnp.float32)


def move_weights(own_normed, gate_weight, up_weight, down_weight):
    normed = lax.all_gather(own_normed, "tp", axis=1, tiled=True)
    gate_acts = jnp.dot(
        normed,
        lax.all_gather(gate_weight, "sp", axis=0, tiled=True),
        preferred_element_type=jnp.float32,
    )
    up_acts = jnp.dot(
        normed,
        lax.all_gather(up_weight, "sp", axis=0, tiled=True),
        preferred_element_type=jnp.float32,
    )
    hidden = (jax.nn.silu(gate_acts) * up_acts).astype(jnp.bfloat16)
    channel_terms = jnp.einsum(
        "df,tf->dt",
        lax.all_gather(down_weight, "sp", axis=0, tiled=True),
        hidden,
        preferred_element_type=jnp.float32,
    )
    channel = lax.psum_scatter(
        channel_terms.astype(jnp.bfloat16), "tp", scatter_dimension=0, tiled=True
    ).astype(jnp.float32)
    return channel.T


def solution(mesh):
    return jax.shard_map(
        local,
        mesh=mesh,
        in_specs=(
            P("sp", "tp"),
            P("sp", "tp"),
            P("sp", "tp"),
            P("tp", "sp"),
            P("tp", "sp"),
            P("sp", "tp"),
            P(),
            P(None, "tp"),
            P(),
            P("sp", "tp"),
            P("sp", "tp"),
            P("sp", "tp"),
        ),
        out_specs=P("sp", "tp"),
        check_vma=False,
    )
```

```python
import functools

import jax
import jax.numpy as jnp
from jax import lax
from jax.experimental import pallas as pl
from jax.experimental.pallas import tpu as pltpu
from jax.sharding import PartitionSpec as P

D = 2048
HEAD_DIM = 128
BLOCK = 128


norm_eps = 1e-06
far_below = -1e30


def entering_state(total):
    memory, top, fall = total
    devices, here = (lax.axis_size("sp"), lax.axis_index("sp"))
    heads, rows, columns = memory.shape
    own_tops = jnp.broadcast_to(jnp.stack([top, fall])[None], (devices, 2, heads))
    tops = lax.all_to_all(own_tops, "sp", 0, 0)
    all_top, all_fall = tops[:, 0], tops[:, 1]
    index = jnp.arange(devices)
    between = (index[None, None, :] > jnp.arange(-1, devices)[None, :, None]) & (
        index[None, None, :] < index[:, None, None]
    )
    after = jnp.sum(jnp.where(between[..., None], all_fall[None, None], 0.0), axis=2)
    reach = jnp.concatenate([jnp.zeros((1, heads), jnp.float32), all_top])[None] + after
    earlier = jnp.arange(-1, devices)[None, :, None] < index[:, None, None]
    reach = jnp.where(earlier, reach, -jnp.inf)
    top_in = jnp.max(reach, axis=1)
    share = jnp.exp(reach - top_in[:, None])[:, 1:]
    pieces = lax.all_to_all(
        jnp.transpose(memory.reshape(heads, devices, rows // devices, columns), (1, 0, 2, 3)),
        "sp", 0, 0,
    )
    sums = jnp.einsum("kjh,jhde->khde", share, pieces, precision=lax.Precision.HIGHEST)
    back = lax.all_to_all(sums, "sp", 0, 0)
    memory_in = jnp.transpose(back, (1, 0, 2, 3)).reshape(heads, rows, columns)
    return (memory_in, lax.dynamic_index_in_dim(top_in, here, 0, False), jnp.zeros_like(fall))


def merge_states(earlier, later):
    memory_early, top_early, fall_early = earlier
    memory_late, top_late, fall_late = later
    new_top = jnp.maximum(fall_late + top_early, top_late)
    keep_early = jnp.exp(fall_late + top_early - new_top)
    keep_late = jnp.exp(top_late - new_top)
    memory = keep_early[..., None, None] * memory_early + keep_late[..., None, None] * memory_late
    return (memory, new_top, fall_early + fall_late)


def memory_cell(queries, keys, values, in_gate, forget_gate, own_gain):
    tokens = queries.shape[0]
    local_heads = in_gate.shape[0]
    blocks = tokens // BLOCK
    key_scale = HEAD_DIM ** (-0.5)
    query_blocks = queries.reshape(blocks, BLOCK, local_heads, HEAD_DIM)
    key_blocks = keys.reshape(blocks, BLOCK, local_heads, HEAD_DIM)
    value_blocks = values.reshape(blocks, BLOCK, local_heads, HEAD_DIM)
    gate_blocks = in_gate.reshape(local_heads, blocks, BLOCK)
    cumulative = jnp.cumsum(
        jax.nn.log_sigmoid(forget_gate).reshape(local_heads, blocks, BLOCK), axis=-1
    )
    block_fall = cumulative[..., -1]
    log_weight = block_fall[..., None] - cumulative + gate_blocks
    block_top = jnp.max(log_weight, axis=-1)
    key_weight = jnp.exp(log_weight - block_top[..., None]) * key_scale
    weighted = (jnp.transpose(key_weight, (1, 2, 0))[..., None] * key_blocks).astype(jnp.bfloat16)
    block_memory = jnp.einsum(
        "nshd,nshe->nhde", weighted, value_blocks, preferred_element_type=jnp.float32
    )
    neutral = (
        jnp.zeros((local_heads, HEAD_DIM, HEAD_DIM), jnp.float32),
        jnp.full((local_heads,), far_below, jnp.float32),
        jnp.zeros((local_heads,), jnp.float32),
    )

    def advance(running, summary):
        return (merge_states(running, summary), running)

    device_total, before_block = lax.scan(
        advance, neutral, (block_memory, block_top.T, block_fall.T)
    )
    entering = entering_state(device_total)
    memory_in, top_in, fall_in = merge_states(
        jax.tree.map(lambda member: member[None], entering), before_block
    )
    causal = lax.broadcasted_iota(jnp.int32, (BLOCK, BLOCK), 0) >= lax.broadcasted_iota(
        jnp.int32, (BLOCK, BLOCK), 1
    )
    spread = cumulative[..., :, None] - cumulative[..., None, :] + gate_blocks[..., None, :]
    spread = jnp.where(causal, spread, -jnp.inf)
    carried = cumulative + top_in.T[..., None]
    row_top = jnp.maximum(carried, jnp.max(spread, axis=-1))
    decay_weight = jnp.exp(spread - row_top[..., None])
    scores = jnp.einsum(
        "nthd,nshd->hnts", query_blocks, key_blocks, preferred_element_type=jnp.float32
    )
    weights = (scores * key_scale * decay_weight).astype(jnp.bfloat16)
    inner_part = jnp.einsum(
        "hnts,nshe->nthe", weights, value_blocks, preferred_element_type=jnp.float32
    )
    outer_part = jnp.einsum(
        "nthd,nhde->nthe",
        query_blocks.astype(jnp.float32),
        memory_in,
        precision=lax.Precision.HIGHEST,
    )
    readout = (
        jnp.transpose(jnp.exp(carried - row_top), (1, 2, 0))[..., None] * outer_part + inner_part
    )
    row_scale = lax.rsqrt(jnp.mean(readout * readout, axis=-1, keepdims=True) + norm_eps)
    head_scale = own_gain.reshape(local_heads, HEAD_DIM)
    normed_heads = (readout * row_scale * head_scale).astype(jnp.bfloat16)
    return normed_heads.reshape(tokens, local_heads * HEAD_DIM)


def local(
    queries,
    keys,
    values,
    in_gate,
    forget_gate,
    stream,
    head_gain,
    out_weight,
    norm_gain,
    gate_weight,
    up_weight,
    down_weight,
):
    column_index = lax.axis_index("tp")
    local_width = queries.shape[1]
    own_gain = lax.dynamic_slice_in_dim(head_gain, column_index * local_width, local_width)
    heads_out = memory_cell(queries, keys, values, in_gate, forget_gate, own_gain)
    columns = out_weight.shape[1]
    projected = jnp.dot(
        lax.all_gather(heads_out, "tp", axis=1, tiled=True),
        out_weight,
        preferred_element_type=jnp.float32,
    )
    mixed_stream = stream.astype(jnp.float32) + projected
    squares = lax.psum(jnp.sum(mixed_stream * mixed_stream, axis=1), "tp")
    factor = lax.rsqrt(squares / D + norm_eps)
    own_norm = lax.dynamic_slice_in_dim(norm_gain, column_index * columns, columns)
    own_normed = (mixed_stream * factor[:, None] * own_norm).astype(jnp.bfloat16)
    if (
        lax.axis_size("tp") == 2
        and lax.axis_size("sp") % 4 == 0
        and own_normed.shape[0] % 32 == 0
        and gate_weight.shape[0] % 128 == 0
        and gate_weight.shape[1] // lax.axis_size("sp") % 16 == 0
        and 2 * own_normed.size * lax.axis_size("tp") < 3 * gate_weight.size
    ):
        channel = move_tokens(own_normed, gate_weight, up_weight, down_weight)
    else:
        channel = move_weights(own_normed, gate_weight, up_weight, down_weight)
    return mixed_stream + 0.5 * channel


def move_tokens(own_normed, gate_weight, up_weight, down_weight):
    devices = lax.axis_size("sp")
    rows, units = gate_weight.shape
    own_units = units // devices
    weights = jnp.stack([gate_weight.T, up_weight.T, down_weight.T])
    weights = jnp.transpose(weights.reshape(3, devices, own_units, rows), (1, 0, 2, 3))
    turned = lax.dynamic_slice_in_dim(
        jnp.concatenate([weights, weights]), lax.axis_index("sp"), devices
    )
    dealt = [turned[0]] + [
        lax.ppermute(turned[k], "sp", [(i, (i + k) % devices) for i in range(devices)])
        for k in range(1, devices)
    ]
    return mixer(own_normed, dealt)


def mixer_kernel(
    layers, own_ref, *refs
):
    dealt = refs[: 4 * layers]
    (
        out_ref, w_ref, seen, total, away, arrived, outgoing, half_in, full_in, layer_in,
        send_sem, seen_sem, twin_sem, away_sem, half_sem, full_sem, layer_sem, copy_sem,
    ) = refs[4 * layers :]
    me, core = lax.axis_index("sp"), lax.axis_index("tp")
    rows = own_ref.shape[0]
    part = rows // 2
    cross = me % 4
    layer = me // 4
    x_of, y_of = cross % 2, cross // 2
    by_x, by_y = y_of * 2 + 1 - x_of, (1 - y_of) * 2 + x_of
    far = (1 - y_of) * 2 + 1 - x_of
    layer_at = [(layer + d) % layers for d in range(layers)]
    to_x = {"sp": layer * 4 + by_x}
    to_y = {"sp": layer * 4 + by_y}
    to_twin = {"tp": 1 - core}
    to_layer = [{"sp": at * 4 + cross} for at in layer_at]

    barrier = pltpu.get_barrier_semaphore()
    peers = [to_x, to_y, to_twin] + to_layer[1:]
    for peer in peers:
        pl.semaphore_signal(barrier, inc=1, device_id=peer, device_id_type=pl.DeviceIdType.MESH)
    pl.semaphore_wait(barrier, len(peers))

    sent = []

    def copy(src, dst, sem, peer):
        one = pltpu.make_async_remote_copy(
            src_ref=src, dst_ref=dst, send_sem=send_sem.at[len(sent)], recv_sem=sem,
            device_id=peer, device_id_type=pl.DeviceIdType.MESH,
        )
        one.start()
        sent.append(one)

    def landed(dst, sem):
        pltpu.make_async_remote_copy(
            src_ref=dst, dst_ref=dst, send_sem=send_sem.at[0], recv_sem=sem,
            device_id=to_twin, device_id_type=pl.DeviceIdType.MESH,
        ).wait_recv()

    lo, hi = pl.ds(0, part), pl.ds(part, part)

    def spread(slot, source):
        here = seen.at[slot, core]
        copy(source, here, seen_sem.at[slot, 0], to_x)
        copy(source, here, seen_sem.at[slot, 0], to_y)
        copy(source, here, twin_sem.at[slot], to_twin)

    keep = pltpu.make_async_copy(own_ref, seen.at[me, core], copy_sem)
    keep.start()
    spread(me, own_ref)
    for d in range(1, layers):
        copy(own_ref, seen.at[me, core], seen_sem.at[me, 0], to_layer[d])
    keep.wait()

    count, units, depth = 4 * layers, dealt[0].shape[1], dealt[0].shape[2]
    if units < w_ref.shape[2]:
        w_ref[:, :, units:, :] = jnp.zeros_like(w_ref[:, :, units:, :])
    for k in range(count):
        source = (me + count - k) % count
        lanes = pl.ds(pl.multiple_of((source % (count // 2)) * depth, depth), depth)
        for kind in range(3):
            w_ref[kind, source // (count // 2), pl.ds(0, units), lanes] = dealt[k][kind]

    def gather(d):
        slot = layer_at[d] * 4 + cross
        landed(seen.at[slot, core], seen_sem.at[slot, 0])
        spread(slot, seen.at[slot, core])

    def forward(d):
        base = layer_at[d] * 4
        slot = base + by_x
        landed(seen.at[slot, core], seen_sem.at[slot, 0])
        copy(seen.at[slot, core, lo], seen.at[slot, core, lo], seen_sem.at[slot, 0], to_y)
        copy(seen.at[slot, core], seen.at[slot, core], twin_sem.at[slot], to_twin)
        slot = base + by_y
        landed(seen.at[slot, core], seen_sem.at[slot, 0])
        copy(seen.at[slot, core, hi], seen.at[slot, core, hi], seen_sem.at[slot, 1], to_x)
        copy(seen.at[slot, core], seen.at[slot, core], twin_sem.at[slot], to_twin)

    def finish(d):
        slot = layer_at[d] * 4 + far
        landed(seen.at[slot, core, lo], seen_sem.at[slot, 0])
        landed(seen.at[slot, core, hi], seen_sem.at[slot, 1])
        copy(seen.at[slot, core], seen.at[slot, core], twin_sem.at[slot], to_twin)

    def compute(d):
        base = layer_at[d] * 4
        for q in range(4):
            landed(seen.at[base + q, 1 - core], twin_sem.at[base + q])
        width = own_ref.shape[1]
        contract = (((1,), (1,)), ((), ()))
        acts = []
        for kind in range(2):
            acts.append(sum(
                lax.dot_general(
                    seen[pl.ds(base, 4), h].reshape(4 * rows, width), w_ref[kind, h], contract,
                    preferred_element_type=jnp.float32,
                )
                for h in range(2)
            ))
        hidden = (jax.nn.silu(acts[0]) * acts[1]).astype(jnp.bfloat16)
        away[d] = jnp.dot(
            hidden, w_ref[2, 1 - core], preferred_element_type=jnp.float32
        ).astype(jnp.bfloat16).reshape(4, rows, width)
        copy(away.at[d], arrived.at[d], away_sem.at[d], to_twin)
        total[d] = jnp.dot(
            hidden, w_ref[2, core], preferred_element_type=jnp.float32
        ).reshape(4, rows, width)

    def reduce_far(d):
        landed(arrived.at[d], away_sem.at[d])
        outgoing[d, 0] = (total[d, far] + arrived[d, far].astype(jnp.float32)).astype(jnp.bfloat16)
        copy(outgoing.at[d, 0, lo], half_in.at[d, 0], half_sem.at[d, 0], to_y)
        copy(outgoing.at[d, 0, hi], half_in.at[d, 1], half_sem.at[d, 1], to_x)

    def reduce_near(d):
        for k, (q, peer) in enumerate(((by_x, to_x), (by_y, to_y))):
            span, rest = ((lo, hi), (hi, lo))[k]
            landed(half_in.at[d, k], half_sem.at[d, k])
            outgoing[d, 1 + k, span] = (
                total[d, q, span] + arrived[d, q, span].astype(jnp.float32)
                + half_in[d, k].astype(jnp.float32)
            ).astype(jnp.bfloat16)
            outgoing[d, 1 + k, rest] = (
                total[d, q, rest] + arrived[d, q, rest].astype(jnp.float32)
            ).astype(jnp.bfloat16)
            copy(outgoing.at[d, 1 + k], full_in.at[d, k], full_sem.at[d, k], peer)

    def reduce_own(d):
        for k in range(2):
            landed(full_in.at[d, k], full_sem.at[d, k])
        own = total[d, cross] + arrived[d, cross].astype(jnp.float32)
        own = own + full_in[d, 0].astype(jnp.float32) + full_in[d, 1].astype(jnp.float32)
        if d == 0:
            out_ref[...] = own
        else:
            outgoing[d, 3] = own.astype(jnp.bfloat16)
            copy(outgoing.at[d, 3], layer_in.at[layer], layer_sem.at[layer], to_layer[d])

    order = [(d + 1) % layers for d in range(layers)]

    def bring(step):
        if step < layers:
            if order[step]:
                gather(order[step])
            forward(order[step])

    bring(0)
    bring(1)
    for step in range(layers + 2):
        if step < layers:
            finish(order[step])
            compute(order[step])
            bring(step + 2)
            reduce_far(order[step])
        if 1 <= step <= layers:
            reduce_near(order[step - 1])
        if step >= 2:
            reduce_own(order[step - 2])
    for d in range(1, layers):
        landed(layer_in.at[layer_at[d]], layer_sem.at[layer_at[d]])
        out_ref[...] += layer_in[layer_at[d]].astype(jnp.float32)
    for one in sent:
        one.wait_send()


def mixer(own_normed, dealt):
    devices = lax.axis_size("sp")
    layers = devices // 4
    rows, width = own_normed.shape
    padded = -(-dealt[0].shape[1] // 128) * 128
    wire, full = jnp.bfloat16, jnp.float32
    dma = pltpu.SemaphoreType.DMA
    return pl.pallas_call(
        functools.partial(mixer_kernel, layers),
        out_shape=jax.ShapeDtypeStruct((rows, width), full),
        in_specs=[pl.BlockSpec(memory_space=pltpu.VMEM)] * (1 + devices),
        out_specs=pl.BlockSpec(memory_space=pltpu.VMEM),
        scratch_shapes=[
            pltpu.VMEM((3, 2, padded, width), wire),
            pltpu.VMEM((devices, 2, rows, width), wire),
            pltpu.VMEM((layers, 4, rows, width), full),
            pltpu.VMEM((layers, 4, rows, width), wire),
            pltpu.VMEM((layers, 4, rows, width), wire),
            pltpu.VMEM((layers, 4, rows, width), wire),
            pltpu.VMEM((layers, 2, rows // 2, width), wire),
            pltpu.VMEM((layers, 2, rows, width), wire),
            pltpu.VMEM((layers, rows, width), wire),
            dma((16 * layers,)),
            dma((devices, 2)),
            dma((devices,)),
            dma((layers,)),
            dma((layers, 2)),
            dma((layers, 2)),
            dma((layers,)),
            dma,
        ],
        compiler_params=pltpu.CompilerParams(
            collective_id=0, has_side_effects=True, vmem_limit_bytes=60 * 2**20
        ),
        cost_estimate=pl.CostEstimate(
            flops=12 * devices * rows * width * padded,
            bytes_accessed=2 * devices * dealt[0].size, transcendentals=0,
        ),
    )(own_normed, *dealt)


def move_weights(own_normed, gate_weight, up_weight, down_weight):
    normed = lax.all_gather(own_normed, "tp", axis=1, tiled=True)
    gate_acts = jnp.dot(
        normed,
        lax.all_gather(gate_weight, "sp", axis=0, tiled=True),
        preferred_element_type=jnp.float32,
    )
    up_acts = jnp.dot(
        normed,
        lax.all_gather(up_weight, "sp", axis=0, tiled=True),
        preferred_element_type=jnp.float32,
    )
    hidden = (jax.nn.silu(gate_acts) * up_acts).astype(jnp.bfloat16)
    channel_terms = jnp.einsum(
        "df,tf->dt",
        lax.all_gather(down_weight, "sp", axis=0, tiled=True),
        hidden,
        preferred_element_type=jnp.float32,
    )
    channel = lax.psum_scatter(
        channel_terms.astype(jnp.bfloat16), "tp", scatter_dimension=0, tiled=True
    ).astype(jnp.float32)
    return channel.T


def solution(mesh):
    return jax.shard_map(
        local,
        mesh=mesh,
        in_specs=(
            P("sp", "tp"),
            P("sp", "tp"),
            P("sp", "tp"),
            P("tp", "sp"),
            P("tp", "sp"),
            P("sp", "tp"),
            P(),
            P(None, "tp"),
            P(),
            P("sp", "tp"),
            P("sp", "tp"),
            P("sp", "tp"),
        ),
        out_specs=P("sp", "tp"),
        check_vma=False,
    )
```
